32 devices in a mesh: sp: 8 (over z, x), tp: 4 (over y, core).
Axes of the slice: x: 2, y: 2, z: 4, core: 2. Of those that a mesh axis runs over, the one named last changes fastest.
Arguments:
- target: bfloat16 [1024, 4096], P('sp', 'tp'), may hold values from -300 to 300
- gain: float32 [4096], P('tp'), may hold values from 0.1 to 1.9
- w_query: bfloat16 [4096, 4096], P('tp'), may hold values from -0.09375 to 0.09375
- queries: bfloat16 [1024, 4096], P('sp', 'tp'), may hold values from -13 to 13
- keys: bfloat16 [4096, 1024], P('sp'), may hold values from -4 to 4
- values: bfloat16 [4096, 1024], P('sp'), may hold values from -4 to 4
- attn_out: bfloat16 [1024, 4096], P('sp', 'tp'), may hold values from -4 to 4
- grad_out: bfloat16 [1024, 4096], P('sp', 'tp'), may hold values from -64 to 64
Outputs:
- grad_rows: bfloat16 [1024, 4096], P('sp', 'tp')
- grad_weight: float32 [4096, 4096], P(('tp', 'sp'))
- grad_keys: float32 [4096, 1024], P(('sp', 'tp'))
- grad_values: float32 [4096, 1024], P(('sp', 'tp'))
The draws below stay inside these ranges and needn't reach their ends.
All inputs are finite; a program needn't handle non-finite values.
Results may differ from the reference program's by a relative error of at most 0.018.
Values may be sent and summed in bfloat16 or wider, within the bound.
A program may use at most 64 MiB of HBM per device.

```python
import math
import jax
import jax.numpy as jnp
from jax import lax

WIDTH = 4096
HEADS = 16
KV_HEADS = 4
HEAD_DIM = 256
TARGET_ROWS = 1024
SOURCE_ROWS = 4096


def draw_target(key, part):
    base_key = jax.random.fold_in(key, 11)
    row_key = jax.random.fold_in(key, 12)
    col_key = jax.random.fold_in(key, 13)
    array_shape = (TARGET_ROWS, WIDTH)
    base_draw = jnp.clip(jax.random.normal(base_key, array_shape, jnp.float32), -4.0, 4.0)
    row_scale = jnp.exp(jax.random.uniform(row_key, (TARGET_ROWS, 1), jnp.float32, 0.0, math.log(10.0)))
    column_ramp = jnp.exp(math.log(5.0) * jnp.arange(WIDTH, dtype=jnp.float32) / WIDTH)
    col_scale = column_ramp * jax.random.uniform(col_key, (WIDTH,), jnp.float32, 0.5, 1.5)
    return (base_draw * row_scale * col_scale).astype(jnp.bfloat16)


def draw_keys(key, part):
    base_key = jax.random.fold_in(key, 21)
    array_shape = (SOURCE_ROWS, KV_HEADS * HEAD_DIM)
    drawn = jnp.clip(jax.random.normal(base_key, array_shape, jnp.float32), -4.0, 4.0)
    return drawn.astype(jnp.bfloat16)


def draw_queries(key, part):
    base_key = jax.random.fold_in(key, 31)
    array_shape = (TARGET_ROWS, HEADS * HEAD_DIM)
    drawn = jnp.clip(jax.random.normal(base_key, array_shape, jnp.float32), -4.0, 4.0)
    return drawn.astype(jnp.bfloat16)


def steps_of(stream_key, shape, cuts, low, top_value):
    level, own = 1.0, jax.random.fold_in(stream_key, 6)
    for axis_at, shards_of in cuts:
        heights = jnp.exp(jax.random.uniform(jax.random.fold_in(own, axis_at), (shards_of,), jnp.float32, low / len(cuts), top_value / len(cuts)))
        level = level * jnp.repeat(heights, shape[axis_at] // shards_of).reshape([-1 if axis == axis_at else 1 for axis in range(len(shape))])
    return level


def scatter_about(own_key, dims, scale, limit, shards=(), held_as=jnp.bfloat16):
    level = steps_of(own_key, dims, shards, -0.22, 0.18) if shards else 1.0
    values = jax.random.normal(own_key, dims, jnp.float32) * scale * level
    return jnp.minimum(jnp.maximum(values, -limit), limit).astype(held_as)


def setup_inputs(seed: int = 0) -> dict:
    seeds = jax.random.split(jax.random.key(seed), 9)
    return {
        "target": draw_target(jax.random.fold_in(seeds[8], 71), 0),
        "gain": jnp.clip(1.0 + 0.18 * jax.random.normal(seeds[1], (WIDTH,), jnp.float32), 0.1, 1.9),
        "w_query": scatter_about(seeds[2], (WIDTH, HEADS * HEAD_DIM), WIDTH ** -0.5, 0.09375, ((0, 4),)),
        "queries": draw_queries(jax.random.fold_in(seeds[8], 71), 0),
        "keys": draw_keys(jax.random.fold_in(seeds[8], 71), 0),
        "values": scatter_about(seeds[5], (SOURCE_ROWS, KV_HEADS * HEAD_DIM), 1.0, 4.0, ((0, 8),)),
        "attn_out": scatter_about(seeds[6], (TARGET_ROWS, HEADS * HEAD_DIM), 1.0, 4.0, ((0, 8), (1, 4))),
        "grad_out": scatter_about(seeds[7], (TARGET_ROWS, HEADS * HEAD_DIM), 16.0, 64.0, ((0, 8), (1, 4))),
    }


norm_eps = 1e-06

def reference(target, gain, w_query, queries, keys, values, attn_out, grad_out):
    target_wide = target.astype(jnp.float32)
    inverse = lax.rsqrt(lax.optimization_barrier(jnp.mean(target_wide * target_wide, axis=1)) + norm_eps)
    normed = (target_wide * inverse[:, None] * gain).astype(jnp.bfloat16)
    group_size = HEADS // KV_HEADS
    score_scale = HEAD_DIM ** (-0.5)
    row_count = queries.shape[0]
    source_count = keys.shape[0]
    query_heads = queries.reshape(row_count, HEADS, HEAD_DIM).transpose(1, 0, 2)
    grad_heads = grad_out.reshape(row_count, HEADS, HEAD_DIM).transpose(1, 0, 2)
    out_heads = attn_out.reshape(row_count, HEADS, HEAD_DIM).transpose(1, 0, 2)
    deltas = lax.optimization_barrier(jnp.sum(grad_heads.astype(jnp.float32) * out_heads.astype(jnp.float32), axis=2))
    head_ids = jnp.arange(HEADS, dtype=jnp.int32)

    def one_head(inputs):
        query_head, grad_head, delta_head, head_id = inputs
        kv_start = (head_id // group_size * HEAD_DIM).astype(jnp.int32)
        key_head = lax.dynamic_slice_in_dim(keys, kv_start, HEAD_DIM, 1)
        value_head = lax.dynamic_slice_in_dim(values, kv_start, HEAD_DIM, 1)
        scores = jnp.dot(query_head, key_head.T, preferred_element_type=jnp.float32) * score_scale
        row_peak = lax.optimization_barrier(jnp.max(scores, axis=1))
        log_totals = row_peak + jnp.log(lax.optimization_barrier(jnp.sum(jnp.exp(scores - row_peak[:, None]), axis=1)))
        weights = jnp.exp(scores - log_totals[:, None])
        weights_rounded = weights.astype(jnp.bfloat16)
        grad_weights = jnp.dot(grad_head, value_head.T, preferred_element_type=jnp.float32)
        grad_scores = (weights * (grad_weights - delta_head[:, None]) * score_scale).astype(jnp.bfloat16)
        query_part = jnp.dot(grad_scores, key_head, preferred_element_type=jnp.float32)
        key_part = jnp.dot(grad_scores.T, query_head, preferred_element_type=jnp.float32)
        value_part = jnp.dot(weights_rounded.T, grad_head, preferred_element_type=jnp.float32)
        return (query_part, key_part, value_part)
    query_parts, key_parts, value_parts = lax.map(one_head, (query_heads, grad_heads, deltas, head_ids))
    query_grad = query_parts.astype(jnp.bfloat16).transpose(1, 0, 2).reshape(row_count, HEADS * HEAD_DIM)
    grad_keys = key_parts.reshape(KV_HEADS, group_size, source_count, HEAD_DIM).sum(axis=1)
    grad_keys = grad_keys.transpose(1, 0, 2).reshape(source_count, KV_HEADS * HEAD_DIM)
    grad_values = value_parts.reshape(KV_HEADS, group_size, source_count, HEAD_DIM).sum(axis=1)
    grad_values = grad_values.transpose(1, 0, 2).reshape(source_count, KV_HEADS * HEAD_DIM)
    grad_rows = jnp.dot(query_grad, w_query.T, preferred_element_type=jnp.float32).astype(jnp.bfloat16)
    grad_weight = jnp.dot(normed.T, query_grad, preferred_element_type=jnp.float32)
    return (grad_rows, grad_weight, grad_keys, grad_values)
```

```python
import functools
import math

import jax
import jax.numpy as jnp
from jax import lax
from jax.experimental import pallas as pl
from jax.experimental.pallas import tpu as pltpu
from jax.sharding import PartitionSpec as P

WIDTH = 4096
HEADS = 16
KV_HEADS = 4
HEAD_DIM = 256


norm_eps = 1e-06


def merged(part, axis, combine):
    gathered = jax.tree.map(lambda a: lax.all_gather(a, axis), part)

    def take(source):
        return jax.tree.map(lambda a: lax.dynamic_index_in_dim(a, source, 0, False), gathered)

    return lax.fori_loop(
        1, lax.axis_size(axis), lambda source, state: combine(state, take(source)), take(0)
    )


def join_stats(first_part, second_part):
    row_peak = jnp.maximum(first_part[0], second_part[0])
    summed = first_part[1] * jnp.exp(first_part[0] - row_peak) + second_part[1] * jnp.exp(
        second_part[0] - row_peak
    )
    return (row_peak, summed, first_part[2] + second_part[2])


def local(target, gain, w_query, queries, keys, values, attn_out, grad_out):
    local_heads = queries.shape[1] // HEAD_DIM
    group_size = HEADS // KV_HEADS
    score_scale = HEAD_DIM ** (-0.5)
    own_rows = queries.shape[0]
    src_rows = keys.shape[0]
    kv_index = lax.axis_index("tp") * local_heads // group_size
    key_own = lax.dynamic_slice_in_dim(keys, kv_index * HEAD_DIM, HEAD_DIM, 1)
    value_own = lax.dynamic_slice_in_dim(values, kv_index * HEAD_DIM, HEAD_DIM, 1)
    out_heads = attn_out.reshape(own_rows, local_heads, HEAD_DIM).astype(jnp.float32)
    grad_heads = grad_out.reshape(own_rows, local_heads, HEAD_DIM).astype(jnp.float32)
    delta_own = jnp.sum(out_heads * grad_heads, axis=2)
    empty_sum = jnp.zeros((src_rows, HEAD_DIM), jnp.float32)
    total_rows = own_rows * lax.axis_size("sp")
    position = lax.axis_index("sp") * own_rows
    delta_full = lax.dynamic_update_slice_in_dim(
        jnp.zeros((total_rows, local_heads), jnp.float32), delta_own, position, 0
    )
    query_all, grad_all = (
        lax.all_gather(queries, "sp", axis=0, tiled=True),
        lax.all_gather(grad_out, "sp", axis=0, tiled=True),
    )
    block_rows = math.gcd(total_rows, 512)
    block_count = total_rows // block_rows
    query_blocks = query_all.reshape(block_count, block_rows, local_heads, HEAD_DIM)
    grad_blocks = grad_all.reshape(block_count, block_rows, local_heads, HEAD_DIM)

    def block_stats(query_block):
        scores = (
            jnp.einsum("qhd,sd->hqs", query_block, key_own, preferred_element_type=jnp.float32)
            * score_scale
        )
        row_peak = jnp.max(scores, axis=2)
        row_total = jnp.sum(jnp.exp(scores - row_peak[:, :, None]), axis=2)
        return (row_peak, row_total)

    peaks, totals = lax.map(block_stats, query_blocks)
    peaks, totals, delta_full = merged((peaks, totals, delta_full), "sp", join_stats)
    log_totals = peaks + jnp.log(totals)
    delta_blocks = delta_full.reshape(block_count, block_rows, local_heads)

    def block_grads(running, inputs):
        query_block, grad_block, delta_block, log_block = inputs
        scores = (
            jnp.einsum("qhd,sd->hqs", query_block, key_own, preferred_element_type=jnp.float32)
            * score_scale
        )
        weights = jnp.exp(scores - log_block[:, :, None])
        grad_weights = jnp.einsum(
            "qhd,sd->hqs", grad_block, value_own, preferred_element_type=jnp.float32
        )
        delta_cols = jnp.transpose(delta_block)
        grad_scores = (weights * (grad_weights - delta_cols[:, :, None]) * score_scale).astype(
            jnp.bfloat16
        )
        key_sum = running[0] + jnp.einsum(
            "hqs,qhd->sd", grad_scores, query_block, preferred_element_type=jnp.float32
        )
        value_sum = running[1] + jnp.einsum(
            "hqs,qhd->sd",
            weights.astype(jnp.bfloat16),
            grad_block,
            preferred_element_type=jnp.float32,
        )
        query_part = jnp.einsum(
            "hqs,sd->qhd", grad_scores, key_own, preferred_element_type=jnp.float32
        )
        return ((key_sum, value_sum), query_part)

    (key_sum, value_sum), query_parts = lax.scan(
        block_grads, (empty_sum, empty_sum), (query_blocks, grad_blocks, delta_blocks, log_totals)
    )
    query_parts = query_parts.reshape(total_rows, 1, local_heads * HEAD_DIM)
    received = lax.all_to_all(
        query_parts.astype(jnp.bfloat16), "sp", split_axis=0, concat_axis=1, tiled=True
    ).astype(query_parts.dtype)
    query_grad = jnp.sum(received, axis=1)
    key_cols = key_sum.reshape(src_rows, 1, HEAD_DIM)
    value_cols = value_sum.reshape(src_rows, 1, HEAD_DIM)
    key_parts, value_parts = (
        lax.all_to_all(
            key_cols.astype(jnp.bfloat16), "tp", split_axis=0, concat_axis=1, tiled=True
        ).astype(key_cols.dtype),
        lax.all_to_all(
            value_cols.astype(jnp.bfloat16), "tp", split_axis=0, concat_axis=1, tiled=True
        ).astype(value_cols.dtype),
    )
    part_rows = key_parts.shape[0]
    per_kv = key_parts.shape[1] // KV_HEADS
    grad_keys = (
        key_parts.reshape(part_rows, KV_HEADS, per_kv, HEAD_DIM)
        .sum(axis=2)
        .reshape(part_rows, KV_HEADS * HEAD_DIM)
    )
    grad_values = (
        value_parts.reshape(part_rows, KV_HEADS, per_kv, HEAD_DIM)
        .sum(axis=2)
        .reshape(part_rows, KV_HEADS * HEAD_DIM)
    )
    query_grad = query_grad.astype(jnp.bfloat16)
    query_all_heads = lax.all_gather(query_grad, "tp", axis=1, tiled=True)
    grad_rows = lax.dot_general(
        query_all_heads, w_query, (((1,), (1,)), ((), ())), preferred_element_type=jnp.float32
    ).astype(jnp.bfloat16)
    target_wide = target.astype(jnp.float32)
    squares = lax.psum(jnp.sum(target_wide * target_wide, axis=1), "tp")
    inverse = lax.rsqrt(squares / WIDTH + norm_eps)
    normed = (target_wide * inverse[:, None] * gain).astype(jnp.bfloat16)
    grad_weight = lax.psum_scatter(
        lax.dot_general(
            normed, query_all_heads, (((0,), (0,)), ((), ())), preferred_element_type=jnp.float32
        ).astype(jnp.bfloat16),
        "sp",
        scatter_dimension=0,
        tiled=True,
    ).astype(jnp.float32)
    return (grad_rows, grad_weight, grad_keys, grad_values)


MESH = pl.DeviceIdType.MESH
BF16, F32 = jnp.bfloat16, jnp.float32
NT = (((1,), (1,)), ((), ()))
X = 2
CHUNK = 256


def fused_kernel(
    zs, ts, heads,
    target, gain, w_query, queries, keys, values, attn_out, grad_out,
    grad_rows, grad_weight, grad_keys, grad_values,
    qs, dos, outs, kbuf, vbuf, ktr, delta, sbuf, pbuf, dsbuf, qpart, qpart_in,
    stat, stat_in, ksum, kv_out, kv_in, kv_tp, kv_tp_in, sq, ntr, nall,
    qg, qt, wbuf, res_out, res_in, send, recv, local_sem,
):
    rows = queries.shape[0]
    src = keys.shape[0]
    hd = HEAD_DIM
    width = heads * hd
    cols = heads * rows
    part = src // ts
    feat = target.shape[1] // (zs * X)
    scale = hd ** (-0.5)
    sp, tp = lax.axis_index("sp"), lax.axis_index("tp")
    z, x = sp // X, sp % X
    counter = [0]
    pending = []

    def zpeer(d, dx=0):
        return (((z + d) % zs) * X + (x + dx) % X, tp)

    def tpeer(e):
        return (sp, (tp + e) % ts)

    def push(source, dest, device):
        i = counter[0]
        counter[0] += 1
        copy = pltpu.make_async_remote_copy(
            src_ref=source, dst_ref=dest, send_sem=send.at[i], recv_sem=recv.at[i],
            device_id=device, device_id_type=MESH,
        )
        copy.start()
        pending.append(copy)
        return copy

    local_count = [0]

    def fetch(source, dest):
        i = local_count[0]
        local_count[0] += 1
        copy = pltpu.make_async_copy(source, dest, local_sem.at[i])
        copy.start()
        return copy

    head_col = pl.ds(pl.multiple_of(tp * hd, hd), hd)
    q_loads, d_loads, o_loads = [], [], []
    kv_loads = [
        fetch(keys.at[:, head_col], kbuf.at[pl.ds(0, src)]),
        fetch(values.at[:, head_col], vbuf.at[pl.ds(0, src)]),
    ]
    for ref, buf, loads in ((queries, qs, q_loads), (grad_out, dos, d_loads), (attn_out, outs, o_loads)):
        for h in range(heads):
            view = buf.at[pl.ds(h * rows, rows)] if buf is outs else buf.at[0, pl.ds(h * rows, rows)]
            loads.append(fetch(ref.at[:, pl.ds(h * hd, hd)], view))
    w_loads = []
    for e in range(ts):
        w_col = pl.ds(pl.multiple_of(((tp + ts - e) % ts) * width, width), width)
        w_loads.append(fetch(w_query.at[:, w_col], wbuf.at[e]))

    barrier = pltpu.get_barrier_semaphore()
    peers = [zpeer(d, dx) for d in range(zs) for dx in range(X) if d + dx]
    peers += [tpeer(e) for e in range(1, ts)]
    for peer in peers:
        pl.semaphore_signal(barrier, inc=1, device_id=peer, device_id_type=MESH)
    pl.semaphore_wait(barrier, len(peers))

    order = [1, zs - 1] + list(range(2, zs - 1)) if zs > 2 else list(range(1, zs))
    for copy in q_loads:
        copy.wait()
    q_in = {d: push(qs.at[0], qs.at[d], zpeer(d)) for d in order}
    for copy in kv_loads:
        copy.wait()
    k_in = push(kbuf.at[pl.ds(0, src)], kbuf.at[pl.ds(src, src)], zpeer(0, 1))
    v_in = push(vbuf.at[pl.ds(0, src)], vbuf.at[pl.ds(src, src)], zpeer(0, 1))
    for copy in d_loads:
        copy.wait()
    do_in = {d: push(dos.at[0], dos.at[d], zpeer(d)) for d in order}

    wide = target[...].astype(F32)
    sq[0] = jnp.broadcast_to(jnp.sum(wide * wide, axis=1, keepdims=True), (rows, 128))
    sq_in = [push(sq.at[0], sq.at[e], tpeer(e)) for e in range(1, ts)]

    for copy in o_loads:
        copy.wait()
    for h in range(heads):
        span = pl.ds(h * rows, rows)
        dot = jnp.sum(dos[0, span].astype(F32) * outs[span].astype(F32), axis=1, keepdims=True)
        delta[0, :, span] = jnp.broadcast_to(dot, (rows, 128)).T[:8]
    delta_in = {d: push(delta.at[0], delta.at[d], zpeer(d)) for d in order}

    for copy in sq_in:
        copy.wait_recv()
    total = sq[0]
    for e in range(1, ts):
        total = total + sq[e]
    inverse = lax.rsqrt(total[:, :1] / (target.shape[1] * ts) + norm_eps)
    normed = target[...].astype(F32) * inverse * gain[...]
    ntr[...] = normed.T.astype(BF16)

    def feature_rows(d, dx):
        owner = ((z + d) % zs) * X + (x + dx) % X
        return pl.ds(pl.multiple_of(owner * feat, feat), feat)

    n_in = []
    for d in range(zs):
        for dx in range(X):
            lanes = pl.ds((d * X + dx) * rows, rows)
            if d + dx:
                n_in.append(
                    push(ntr.at[feature_rows(d, dx)], nall.at[0, :, lanes], zpeer(d, dx))
                )
            else:
                nall[0, :, lanes] = ntr[feature_rows(0, 0)]

    ktr[:, :src] = kbuf[:src].T
    k_in.wait_recv()
    ktr[:, src:] = kbuf[src:].T
    v_in.wait_recv()
    chunks = X * src // CHUNK

    def scores_of(d):
        def step(c, peak):
            span = pl.ds(pl.multiple_of(c * CHUNK, CHUNK), CHUNK)
            s = lax.dot_general(kbuf[span], qs[d], NT, preferred_element_type=F32)
            sbuf[span] = s
            return jnp.maximum(peak, jnp.max(s, axis=0, keepdims=True))

        return lax.fori_loop(0, chunks, step, jnp.full((1, cols), -jnp.inf, F32))

    def grads_of(d, peak):
        own_delta = delta[d, :1]

        def step(c, total):
            span = pl.ds(pl.multiple_of(c * CHUNK, CHUNK), CHUNK)
            p = jnp.exp((sbuf[span] - peak) * scale)
            dp = lax.dot_general(vbuf[span], dos[d], NT, preferred_element_type=F32)
            pbuf[d, span] = p.astype(BF16)
            dsbuf[d, span] = (p * (dp - own_delta) * scale).astype(BF16)
            return total + jnp.sum(p, axis=0, keepdims=True)

        total = lax.fori_loop(0, chunks, step, jnp.zeros((1, cols), F32))
        stat[d, 0:1] = peak * scale
        stat[d, 1:2] = total
        stat[d, 2:8] = jnp.zeros((6, cols), F32)
        return jnp.dot(ktr[...], dsbuf[d], preferred_element_type=F32)

    qp_in, own_part = {}, None
    for d in [0] + order:
        if d:
            q_in[d].wait_recv()
        peak = scores_of(d)
        if d:
            do_in[d].wait_recv()
            delta_in[d].wait_recv()
        part_t = grads_of(d, peak)
        qpart[d] = part_t.astype(BF16)
        if d:
            qp_in[d] = push(qpart.at[d], qpart_in.at[d], zpeer(zs - d))
        if d == 0:
            for copy in n_in:
                copy.wait_recv()
            nt_in = [push(nall.at[0], nall.at[e], tpeer(e)) for e in range(1, ts)]

    stat_copies = [push(stat, stat_in.at[d], zpeer(d)) for d in order]
    for copy in stat_copies:
        copy.wait_recv()

    def stats_of(d, e):
        ref = stat.at[d] if e == 0 else stat_in.at[e, (d + zs - e) % zs]
        return ref[0:1], ref[1:2]

    def ratios(d):
        parts = [stats_of(d, e) for e in range(zs)]
        top = parts[0][0]
        for m, _ in parts[1:]:
            top = jnp.maximum(top, m)
        factors = [jnp.exp(m - top) for m, _ in parts]
        summed = sum(f * l for f, (_, l) in zip(factors, parts))
        return [f / summed for f in factors]

    own_ratios = ratios(0)
    for d in range(zs):
        r = own_ratios[0] if d == 0 else ratios(d)[0]
        r = jnp.broadcast_to(r, (128, cols)).T
        r = jnp.concatenate([r] * (hd // 128), axis=1)
        sbuf_q = (qs[d].astype(F32) * r).astype(BF16)
        sbuf_d = (dos[d].astype(F32) * r).astype(BF16)
        for i, (left, right) in enumerate(((dsbuf, sbuf_q), (pbuf, sbuf_d))):
            piece = jnp.dot(left[d], right, preferred_element_type=F32)
            ksum[i] = piece if d == 0 else ksum[i] + piece
    kv_out[...] = ksum[:, src:].astype(BF16)
    kvx_in = push(kv_out, kv_in, zpeer(0, 1))

    grad_t = qpart[0].astype(F32) * own_ratios[0]
    for d in order:
        qp_in[d].wait_recv()
        grad_t = grad_t + qpart_in[d].astype(F32) * own_ratios[(zs - d) % zs]
    grad_own = grad_t.T
    for h in range(heads):
        qg[pl.ds(0, rows), pl.ds(h * hd, hd)] = grad_own[h * rows : (h + 1) * rows].astype(BF16)
    own = qg.at[pl.ds(0, rows)]
    slot = lambda d, dx: qg.at[pl.ds((d * X + dx) * rows, rows)]
    qz_in = {d: push(own, slot(d, 0), zpeer(d)) for d in order}
    qx_in = {0: push(own, slot(0, 1), zpeer(0, 1))}
    qt_in = {e: push(own, qt.at[e], tpeer(e)) for e in range(1, ts)}

    kvx_in.wait_recv()
    for i in range(2):
        ksum[i, :src] = ksum[i, :src] + kv_in[i].astype(F32)
    kv_tp[...] = ksum[:, :src].astype(BF16)

    def part_rows(e):
        return pl.ds(pl.multiple_of(((tp + e) % ts) * part, part), part)

    kvt_in = [push(kv_tp.at[:, part_rows(e)], kv_tp_in.at[e], tpeer(e)) for e in range(1, ts)]
    for i, out in enumerate((grad_keys, grad_values)):
        out[:, head_col] = ksum[i, part_rows(0)]

    for d in order[:2]:
        qz_in[d].wait_recv()
        qx_in[d] = push(slot(d, 0), slot(d, 1), zpeer(0, 1))
    w_loads[0].wait()
    rows_sum = lax.dot_general(own[...], wbuf[0], NT, preferred_element_type=F32)
    for e in range(1, ts):
        qt_in[e].wait_recv()
        w_loads[e].wait()
        rows_sum = rows_sum + lax.dot_general(qt[e], wbuf[e], NT, preferred_element_type=F32)
    grad_rows[...] = rows_sum.astype(BF16)
    for d in order[2:]:
        qz_in[d].wait_recv()
        qx_in[d] = push(slot(d, 0), slot(d, 1), zpeer(0, 1))
    for e in range(1, ts):
        kvt_in[e - 1].wait_recv()
        at = pl.ds(pl.multiple_of(((tp + ts - e) % ts) * hd, hd), hd)
        for i, out in enumerate((grad_keys, grad_values)):
            out[:, at] = kv_tp_in[e, i].astype(F32)
    for copy in nt_in:
        copy.wait_recv()
    for d in [0] + order:
        qx_in[d].wait_recv()
    res_copies = {}
    for e in [*range(1, ts), 0]:
        piece = jnp.dot(nall[e], qg[...], preferred_element_type=F32)
        if e:
            res_out[e] = piece.astype(BF16)
            res_copies[e] = push(res_out.at[e], res_in.at[e], tpeer(ts - e))
        else:
            grad_weight[:, pl.ds(pl.multiple_of(tp * width, width), width)] = piece
    for e in range(1, ts):
        res_copies[e].wait_recv()
        at = pl.ds(pl.multiple_of(((tp + e) % ts) * width, width), width)
        grad_weight[:, at] = res_in[e].astype(F32)
    for copy in pending:
        copy.wait_send()


def fused(target, gain, w_query, queries, keys, values, attn_out, grad_out):
    zs, ts = lax.axis_size("sp") // X, lax.axis_size("tp")
    rows, width = queries.shape
    src = keys.shape[0]
    heads = width // HEAD_DIM
    cols, hd = heads * rows, HEAD_DIM
    feats = target.shape[1]
    feat = feats // (zs * X)
    part = src // ts
    copies = 6 * zs * X + 8 * ts + 16
    vmem, hbm = pl.BlockSpec(memory_space=pltpu.VMEM), pl.BlockSpec(memory_space=pl.ANY)
    return pl.pallas_call(
        functools.partial(fused_kernel, zs, ts, heads),
        out_shape=(
            jax.ShapeDtypeStruct((rows, feats), BF16),
            jax.ShapeDtypeStruct((feat, width * ts), F32),
            jax.ShapeDtypeStruct((part, keys.shape[1]), F32),
            jax.ShapeDtypeStruct((part, keys.shape[1]), F32),
        ),
        in_specs=[vmem, vmem, hbm, hbm, hbm, hbm, hbm, hbm],
        out_specs=(vmem,) * 4,
        scratch_shapes=[
            pltpu.VMEM((zs, cols, hd), BF16),
            pltpu.VMEM((zs, cols, hd), BF16),
            pltpu.VMEM((cols, hd), BF16),
            pltpu.VMEM((X * src, hd), BF16),
            pltpu.VMEM((X * src, hd), BF16),
            pltpu.VMEM((hd, X * src), BF16),
            pltpu.VMEM((zs, 8, cols), F32),
            pltpu.VMEM((X * src, cols), F32),
            pltpu.VMEM((zs, X * src, cols), BF16),
            pltpu.VMEM((zs, X * src, cols), BF16),
            pltpu.VMEM((zs, hd, cols), BF16),
            pltpu.VMEM((zs, hd, cols), BF16),
            pltpu.VMEM((zs, 8, cols), F32),
            pltpu.VMEM((zs, zs, 8, cols), F32),
            pltpu.VMEM((2, X * src, hd), F32),
            pltpu.VMEM((2, src, hd), BF16),
            pltpu.VMEM((2, src, hd), BF16),
            pltpu.VMEM((2, src, hd), BF16),
            pltpu.VMEM((ts, 2, part, hd), BF16),
            pltpu.VMEM((ts, rows, 128), F32),
            pltpu.VMEM((feats, rows), BF16),
            pltpu.VMEM((ts, feat, zs * X * rows), BF16),
            pltpu.VMEM((zs * X * rows, width), BF16),
            pltpu.VMEM((ts, rows, width), BF16),
            pltpu.VMEM((ts, feats, width), BF16),
            pltpu.VMEM((ts, feat, width), BF16),
            pltpu.VMEM((ts, feat, width), BF16),
            pltpu.SemaphoreType.DMA((copies,)),
            pltpu.SemaphoreType.DMA((copies,)),
            pltpu.SemaphoreType.DMA((2 + 3 * heads + ts,)),
        ],
        compiler_params=pltpu.CompilerParams(
            collective_id=0, has_side_effects=True, vmem_limit_bytes=60 * 2**20
        ),
    )(target, gain.reshape(1, feats), w_query, queries, keys, values, attn_out, grad_out)


def fits(mesh):
    sp, tp = mesh.shape["sp"], mesh.shape["tp"]
    feat = WIDTH // (sp * tp)
    return tp == KV_HEADS and sp % X == 0 and sp > X and feat % 128 == 0


def solution(mesh):
    return jax.shard_map(
        fused if fits(mesh) else local,
        mesh=mesh,
        in_specs=(
            P("sp", "tp"),
            P("tp"),
            P("tp", None),
            P("sp", "tp"),
            P("sp", None),
            P("sp", None),
            P("sp", "tp"),
            P("sp", "tp"),
        ),
        out_specs=(
            P("sp", "tp"),
            P(("tp", "sp"), None),
            P(("sp", "tp"), None),
            P(("sp", "tp"), None),
        ),
        check_vma=False,
    )
```

```python
import functools
import math

import jax
import jax.numpy as jnp
from jax import lax
from jax.experimental import pallas as pl
from jax.experimental.pallas import tpu as pltpu
from jax.sharding import PartitionSpec as P

WIDTH = 4096
HEADS = 16
KV_HEADS = 4
HEAD_DIM = 256


norm_eps = 1e-06


def merged(part, axis, combine):
    gathered = jax.tree.map(lambda a: lax.all_gather(a, axis), part)

    def take(source):
        return jax.tree.map(lambda a: lax.dynamic_index_in_dim(a, source, 0, False), gathered)

    return lax.fori_loop(
        1, lax.axis_size(axis), lambda source, state: combine(state, take(source)), take(0)
    )


def join_stats(first_part, second_part):
    row_peak = jnp.maximum(first_part[0], second_part[0])
    summed = first_part[1] * jnp.exp(first_part[0] - row_peak) + second_part[1] * jnp.exp(
        second_part[0] - row_peak
    )
    return (row_peak, summed, first_part[2] + second_part[2])


def local(target, gain, w_query, queries, keys, values, attn_out, grad_out):
    local_heads = queries.shape[1] // HEAD_DIM
    group_size = HEADS // KV_HEADS
    score_scale = HEAD_DIM ** (-0.5)
    own_rows = queries.shape[0]
    src_rows = keys.shape[0]
    kv_index = lax.axis_index("tp") * local_heads // group_size
    key_own = lax.dynamic_slice_in_dim(keys, kv_index * HEAD_DIM, HEAD_DIM, 1)
    value_own = lax.dynamic_slice_in_dim(values, kv_index * HEAD_DIM, HEAD_DIM, 1)
    out_heads = attn_out.reshape(own_rows, local_heads, HEAD_DIM).astype(jnp.float32)
    grad_heads = grad_out.reshape(own_rows, local_heads, HEAD_DIM).astype(jnp.float32)
    delta_own = jnp.sum(out_heads * grad_heads, axis=2)
    empty_sum = jnp.zeros((src_rows, HEAD_DIM), jnp.float32)
    total_rows = own_rows * lax.axis_size("sp")
    position = lax.axis_index("sp") * own_rows
    delta_full = lax.dynamic_update_slice_in_dim(
        jnp.zeros((total_rows, local_heads), jnp.float32), delta_own, position, 0
    )
    query_all, grad_all = (
        lax.all_gather(queries, "sp", axis=0, tiled=True),
        lax.all_gather(grad_out, "sp", axis=0, tiled=True),
    )
    block_rows = math.gcd(total_rows, 512)
    block_count = total_rows // block_rows
    query_blocks = query_all.reshape(block_count, block_rows, local_heads, HEAD_DIM)
    grad_blocks = grad_all.reshape(block_count, block_rows, local_heads, HEAD_DIM)

    def block_stats(query_block):
        scores = (
            jnp.einsum("qhd,sd->hqs", query_block, key_own, preferred_element_type=jnp.float32)
            * score_scale
        )
        row_peak = jnp.max(scores, axis=2)
        row_total = jnp.sum(jnp.exp(scores - row_peak[:, :, None]), axis=2)
        return (row_peak, row_total)

    peaks, totals = lax.map(block_stats, query_blocks)
    peaks, totals, delta_full = merged((peaks, totals, delta_full), "sp", join_stats)
    log_totals = peaks + jnp.log(totals)
    delta_blocks = delta_full.reshape(block_count, block_rows, local_heads)

    def block_grads(running, inputs):
        query_block, grad_block, delta_block, log_block = inputs
        scores = (
            jnp.einsum("qhd,sd->hqs", query_block, key_own, preferred_element_type=jnp.float32)
            * score_scale
        )
        weights = jnp.exp(scores - log_block[:, :, None])
        grad_weights = jnp.einsum(
            "qhd,sd->hqs", grad_block, value_own, preferred_element_type=jnp.float32
        )
        delta_cols = jnp.transpose(delta_block)
        grad_scores = (weights * (grad_weights - delta_cols[:, :, None]) * score_scale).astype(
            jnp.bfloat16
        )
        key_sum = running[0] + jnp.einsum(
            "hqs,qhd->sd", grad_scores, query_block, preferred_element_type=jnp.float32
        )
        value_sum = running[1] + jnp.einsum(
            "hqs,qhd->sd",
            weights.astype(jnp.bfloat16),
            grad_block,
            preferred_element_type=jnp.float32,
        )
        query_part = jnp.einsum(
            "hqs,sd->qhd", grad_scores, key_own, preferred_element_type=jnp.float32
        )
        return ((key_sum, value_sum), query_part)

    (key_sum, value_sum), query_parts = lax.scan(
        block_grads, (empty_sum, empty_sum), (query_blocks, grad_blocks, delta_blocks, log_totals)
    )
    query_parts = query_parts.reshape(total_rows, 1, local_heads * HEAD_DIM)
    received = lax.all_to_all(
        query_parts.astype(jnp.bfloat16), "sp", split_axis=0, concat_axis=1, tiled=True
    ).astype(query_parts.dtype)
    query_grad = jnp.sum(received, axis=1)
    key_cols = key_sum.reshape(src_rows, 1, HEAD_DIM)
    value_cols = value_sum.reshape(src_rows, 1, HEAD_DIM)
    key_parts, value_parts = (
        lax.all_to_all(
            key_cols.astype(jnp.bfloat16), "tp", split_axis=0, concat_axis=1, tiled=True
        ).astype(key_cols.dtype),
        lax.all_to_all(
            value_cols.astype(jnp.bfloat16), "tp", split_axis=0, concat_axis=1, tiled=True
        ).astype(value_cols.dtype),
    )
    part_rows = key_parts.shape[0]
    per_kv = key_parts.shape[1] // KV_HEADS
    grad_keys = (
        key_parts.reshape(part_rows, KV_HEADS, per_kv, HEAD_DIM)
        .sum(axis=2)
        .reshape(part_rows, KV_HEADS * HEAD_DIM)
    )
    grad_values = (
        value_parts.reshape(part_rows, KV_HEADS, per_kv, HEAD_DIM)
        .sum(axis=2)
        .reshape(part_rows, KV_HEADS * HEAD_DIM)
    )
    query_grad = query_grad.astype(jnp.bfloat16)
    query_all_heads = lax.all_gather(query_grad, "tp", axis=1, tiled=True)
    grad_rows = lax.dot_general(
        query_all_heads, w_query, (((1,), (1,)), ((), ())), preferred_element_type=jnp.float32
    ).astype(jnp.bfloat16)
    target_wide = target.astype(jnp.float32)
    squares = lax.psum(jnp.sum(target_wide * target_wide, axis=1), "tp")
    inverse = lax.rsqrt(squares / WIDTH + norm_eps)
    normed = (target_wide * inverse[:, None] * gain).astype(jnp.bfloat16)
    grad_weight = lax.psum_scatter(
        lax.dot_general(
            normed, query_all_heads, (((0,), (0,)), ((), ())), preferred_element_type=jnp.float32
        ).astype(jnp.bfloat16),
        "sp",
        scatter_dimension=0,
        tiled=True,
    ).astype(jnp.float32)
    return (grad_rows, grad_weight, grad_keys, grad_values)


MESH = pl.DeviceIdType.MESH
BF16, F32 = jnp.bfloat16, jnp.float32
NT = (((1,), (1,)), ((), ()))
X = 2
CHUNK = 256


def fused_kernel(
    zs, ts, heads,
    target, gain, w_query, queries, keys, values, attn_out, grad_out,
    grad_rows, grad_weight, grad_keys, grad_values,
    qs, dos, outs, kbuf, vbuf, ktr, delta, sbuf, pbuf, dsbuf, qpart, qpart_in,
    stat, stat_in, ksum, kv_out, kv_in, kv_tp, kv_tp_in, sq, ntr, nall,
    qown, qg, qt, wbuf, res_out, res_in, send, recv, local_sem, zsend, zrecv, psend, precv, qxs, qxr,
):
    rows = queries.shape[0]
    src = keys.shape[0]
    hd = HEAD_DIM
    width = heads * hd
    cols = heads * rows
    part = src // ts
    feat = target.shape[1] // (zs * X)
    scale = hd ** (-0.5)
    sp, tp = lax.axis_index("sp"), lax.axis_index("tp")
    z, x = sp // X, sp % X
    counter = [0]
    pending = []

    def zpeer(d, dx=0):
        return (((z + d) % zs) * X + (x + dx) % X, tp)

    def tpeer(e):
        return (sp, (tp + e) % ts)

    def push(source, dest, device):
        i = counter[0]
        counter[0] += 1
        copy = pltpu.make_async_remote_copy(
            src_ref=source, dst_ref=dest, send_sem=send.at[i], recv_sem=recv.at[i],
            device_id=device, device_id_type=MESH,
        )
        copy.start()
        pending.append(copy)
        return copy

    def run(device, source, dest, ssem, rsem):
        return pltpu.make_async_remote_copy(
            src_ref=source, dst_ref=dest, send_sem=ssem, recv_sem=rsem,
            device_id=device, device_id_type=MESH,
        )

    first = (zs - 1 - z) // (zs - 1)
    last = z // (zs - 1)
    inner = first + last == 0
    near = [1 + 2 * first, 3 - first - last, 2 - first + last]

    def hops(stream, view, d):
        up = run(
            zpeer(1), view(d), view((d + 1) % zs), zsend.at[stream, d, 0],
            zrecv.at[stream, (d + 1) % zs],
        )
        down = run(
            zpeer(zs - 1), view(d), view((d + zs - 1) % zs), zsend.at[stream, d, 1],
            zrecv.at[stream, (d + zs - 1) % zs],
        )
        below, above = z >= d, z < d
        if isinstance(d, int) and d == 0:
            above = z >= 0
        return ((up, below & (z < zs - 1)), (down, above & (z > 0)))

    def forward(stream, view, d):
        for copy, wanted in hops(stream, view, d):
            pl.when(wanted)(copy.start)

    def arrived(stream, view, d):
        run(zpeer(1), view(0), view(d), zsend.at[stream, 0, 0], zrecv.at[stream, d]).wait_recv()

    def relay(stream, view, d):
        arrived(stream, view, d)
        forward(stream, view, d)

    q_view, d_view = (lambda d: qs.at[d]), (lambda d: dos.at[d])
    half = width // 2

    def g_view(b, dx=0):
        return lambda d: qg.at[b, pl.ds(pl.multiple_of((d * X + dx) * rows, rows), rows)]

    streams = ((0, q_view), (1, d_view), (2, g_view(0)), (3, g_view(1)))

    local_count = [0]

    def fetch(source, dest):
        i = local_count[0]
        local_count[0] += 1
        copy = pltpu.make_async_copy(source, dest, local_sem.at[i])
        copy.start()
        return copy

    head_col = pl.ds(pl.multiple_of(tp * hd, hd), hd)
    q_loads, d_loads, o_loads = [], [], []
    kv_loads = [
        fetch(keys.at[:, head_col], kbuf.at[pl.ds(0, src)]),
        fetch(values.at[:, head_col], vbuf.at[pl.ds(0, src)]),
    ]
    for ref, buf, loads in ((queries, qs, q_loads), (grad_out, dos, d_loads), (attn_out, outs, o_loads)):
        for h in range(heads):
            view = buf.at[pl.ds(h * rows, rows)] if buf is outs else buf.at[0, pl.ds(h * rows, rows)]
            loads.append(fetch(ref.at[:, pl.ds(h * hd, hd)], view))
    w_loads = []
    for e in range(ts):
        w_col = pl.ds(pl.multiple_of(((tp + ts - e) % ts) * width, width), width)
        w_loads.append(fetch(w_query.at[:, w_col], wbuf.at[e]))

    barrier = pltpu.get_barrier_semaphore()
    peers = [zpeer(d, dx) for d in range(zs) for dx in range(X) if d + dx]
    peers += [tpeer(e) for e in range(1, ts)]
    for peer in peers:
        pl.semaphore_signal(barrier, inc=1, device_id=peer, device_id_type=MESH)
    pl.semaphore_wait(barrier, len(peers))

    order = [1, zs - 1] + list(range(2, zs - 1)) if zs > 2 else list(range(1, zs))
    for copy in q_loads:
        copy.wait()
    forward(0, q_view, 0)
    for copy in kv_loads:
        copy.wait()
    k_in = push(kbuf.at[pl.ds(0, src)], kbuf.at[pl.ds(src, src)], zpeer(0, 1))
    v_in = push(vbuf.at[pl.ds(0, src)], vbuf.at[pl.ds(src, src)], zpeer(0, 1))
    for copy in d_loads:
        copy.wait()
    forward(1, d_view, 0)

    wide = target[...].astype(F32)
    sq[0] = jnp.broadcast_to(jnp.sum(wide * wide, axis=1, keepdims=True), (rows, 128))
    sq_in = [push(sq.at[0], sq.at[e], tpeer(e)) for e in range(1, ts)]

    for copy in o_loads:
        copy.wait()
    for h in range(heads):
        span = pl.ds(h * rows, rows)
        dot = jnp.sum(dos[0, span].astype(F32) * outs[span].astype(F32), axis=1, keepdims=True)
        delta[0, :, span] = jnp.broadcast_to(dot, (rows, 128)).T[:8]
    delta_in = {d: push(delta.at[0], delta.at[d], zpeer(d)) for d in order}

    for copy in sq_in:
        copy.wait_recv()
    total = sq[0]
    for e in range(1, ts):
        total = total + sq[e]
    inverse = lax.rsqrt(total[:, :1] / (target.shape[1] * ts) + norm_eps)
    normed = target[...].astype(F32) * inverse * gain[...]
    ntr[...] = normed.T.astype(BF16)

    def feature_rows(d, dx):
        owner = ((z + d) % zs) * X + (x + dx) % X
        return pl.ds(pl.multiple_of(owner * feat, feat), feat)

    n_in = []
    for d in range(zs):
        for dx in range(X):
            lanes = pl.ds((d * X + dx) * rows, rows)
            if d + dx:
                n_in.append(
                    push(ntr.at[feature_rows(d, dx)], nall.at[0, :, lanes], zpeer(d, dx))
                )
            else:
                nall[0, :, lanes] = ntr[feature_rows(0, 0)]

    chunks = X * src // CHUNK

    def scores_of(d):
        def step(c, peak):
            span = pl.ds(pl.multiple_of(c * CHUNK, CHUNK), CHUNK)
            s = lax.dot_general(kbuf[span], qs[d], NT, preferred_element_type=F32)
            sbuf[span] = s
            return jnp.maximum(peak, jnp.max(s, axis=0, keepdims=True))

        return lax.fori_loop(0, chunks, step, jnp.full((1, cols), -jnp.inf, F32))

    def grads_of(d, peak):
        own_delta = delta[d, :1]

        def step(c, total):
            span = pl.ds(pl.multiple_of(c * CHUNK, CHUNK), CHUNK)
            p = jnp.exp((sbuf[span] - peak) * scale)
            dp = lax.dot_general(vbuf[span], dos[d], NT, preferred_element_type=F32)
            pbuf[d, span] = p.astype(BF16)
            dsbuf[d, span] = (p * (dp - own_delta) * scale).astype(BF16)
            return total + jnp.sum(p, axis=0, keepdims=True)

        total = lax.fori_loop(0, chunks, step, jnp.zeros((1, cols), F32))
        stat[d, 0:1] = peak * scale
        stat[d, 1:2] = total
        stat[d, 2:8] = jnp.zeros((6, cols), F32)
        return jnp.dot(ktr[...], dsbuf[d], preferred_element_type=F32)

    def process(d):
        peak = scores_of(d)
        qpart[d] = grads_of(d, peak).astype(BF16)

    def part_copy(d):
        return run(zpeer(zs - d), qpart.at[d], qpart_in.at[d], psend.at[d], precv.at[d])

    relay(0, q_view, near[0])
    ktr[:, :src] = kbuf[:src].T
    k_in.wait_recv()
    ktr[:, src:] = kbuf[src:].T
    relay(1, d_view, near[0])
    v_in.wait_recv()

    @pl.when(inner)
    def _():
        relay(0, q_view, near[1])
        relay(1, d_view, near[1])

    for copy in delta_in.values():
        copy.wait_recv()
    process(0)

    @pl.when(inner)
    def _():
        relay(0, q_view, near[2])

    process(near[0])
    part_copy(near[0]).start()

    @pl.when(inner)
    def _():
        relay(1, d_view, near[2])

    @pl.when(first + last > 0)
    def _():
        arrived(0, q_view, near[1])
        arrived(1, d_view, near[1])

    process(near[1])
    part_copy(near[1]).start()

    @pl.when(first + last > 0)
    def _():
        arrived(0, q_view, near[2])
        arrived(1, d_view, near[2])

    process(near[2])
    part_copy(near[2]).start()
    for copy in n_in:
        copy.wait_recv()
    nt_in = [push(nall.at[0], nall.at[e], tpeer(e)) for e in range(1, ts)]

    stat_copies = [push(stat, stat_in.at[d], zpeer(d)) for d in order]
    for copy in stat_copies:
        copy.wait_recv()

    def stats_of(d, e):
        ref = stat.at[d] if e == 0 else stat_in.at[e, (d + zs - e) % zs]
        return ref[0:1], ref[1:2]

    def ratios(d):
        parts = [stats_of(d, e) for e in range(zs)]
        top = parts[0][0]
        for m, _ in parts[1:]:
            top = jnp.maximum(top, m)
        factors = [jnp.exp(m - top) for m, _ in parts]
        summed = sum(f * l for f, (_, l) in zip(factors, parts))
        return [f / summed for f in factors]

    own_ratios = ratios(0)
    for d in range(zs):
        r = own_ratios[0] if d == 0 else ratios(d)[0]
        r = jnp.broadcast_to(r, (128, cols)).T
        r = jnp.concatenate([r] * (hd // 128), axis=1)
        sbuf_q = (qs[d].astype(F32) * r).astype(BF16)
        sbuf_d = (dos[d].astype(F32) * r).astype(BF16)
        for i, (left, right) in enumerate(((dsbuf, sbuf_q), (pbuf, sbuf_d))):
            piece = jnp.dot(left[d], right, preferred_element_type=F32)
            ksum[i] = piece if d == 0 else ksum[i] + piece
    kv_out[...] = ksum[:, src:].astype(BF16)
    kvx_in = push(kv_out, kv_in, zpeer(0, 1))

    grad_t = qpart[0].astype(F32) * own_ratios[0]
    for d in order:
        part_copy(d).wait_recv()
        grad_t = grad_t + qpart_in[d].astype(F32) * own_ratios[(zs - d) % zs]
    grad_own = grad_t.T
    for h in range(heads):
        piece = grad_own[h * rows : (h + 1) * rows].astype(BF16)
        qown[:, pl.ds(h * hd, hd)] = piece
        b, at = h * hd // half, h * hd % half
        qg[b, pl.ds(0, rows), pl.ds(at, hd)] = piece
    def cross(b, d):
        run(zpeer(0, 1), g_view(b)(d), g_view(b, 1)(d), qxs.at[b, d], qxr.at[b, d]).start()

    forward(2, g_view(0), 0)
    cross(0, 0)
    qt_in = {e: push(qown, qt.at[e], tpeer(e)) for e in range(1, ts)}
    relay(2, g_view(0), near[0])
    forward(3, g_view(1), 0)
    cross(0, near[0])
    cross(1, 0)

    kvx_in.wait_recv()
    for i in range(2):
        ksum[i, :src] = ksum[i, :src] + kv_in[i].astype(F32)
    kv_tp[...] = ksum[:, :src].astype(BF16)

    def part_rows(e):
        return pl.ds(pl.multiple_of(((tp + e) % ts) * part, part), part)

    kvt_in = [push(kv_tp.at[:, part_rows(e)], kv_tp_in.at[e], tpeer(e)) for e in range(1, ts)]
    for i, out in enumerate((grad_keys, grad_values)):
        out[:, head_col] = ksum[i, part_rows(0)]

    w_loads[0].wait()
    rows_sum = lax.dot_general(qown[...], wbuf[0], NT, preferred_element_type=F32)
    relay(2, g_view(0), near[1])
    cross(0, near[1])
    relay(3, g_view(1), near[0])
    cross(1, near[0])
    relay(2, g_view(0), near[2])
    cross(0, near[2])
    relay(3, g_view(1), near[1])
    cross(1, near[1])
    for e in range(1, ts):
        kvt_in[e - 1].wait_recv()
        at = pl.ds(pl.multiple_of(((tp + ts - e) % ts) * hd, hd), hd)
        for i, out in enumerate((grad_keys, grad_values)):
            out[:, at] = kv_tp_in[e, i].astype(F32)
    for copy in nt_in:
        copy.wait_recv()
    def crossed(b):
        for d in range(zs):
            run(zpeer(0, 1), g_view(b)(d), g_view(b, 1)(d), qxs.at[b, d], qxr.at[b, d]).wait_recv()

    res_copies = {}

    def project(b):
        for e in [*range(1, ts), 0]:
            piece = jnp.dot(nall[e], qg[b], preferred_element_type=F32)
            if e:
                res_out[b, e] = piece.astype(BF16)
                res_copies[b, e] = push(res_out.at[b, e], res_in.at[b, e], tpeer(ts - e))
            else:
                grad_weight[:, pl.ds(pl.multiple_of(tp * width + b * half, half), half)] = piece

    crossed(0)
    project(0)
    relay(3, g_view(1), near[2])
    cross(1, near[2])
    for e in range(1, ts):
        qt_in[e].wait_recv()
        w_loads[e].wait()
        rows_sum = rows_sum + lax.dot_general(qt[e], wbuf[e], NT, preferred_element_type=F32)
    grad_rows[...] = rows_sum.astype(BF16)
    crossed(1)
    project(1)
    for b in range(2):
        for e in range(1, ts):
            res_copies[b, e].wait_recv()
            at = ((tp + e) % ts) * width + b * half
            grad_weight[:, pl.ds(pl.multiple_of(at, half), half)] = res_in[b, e].astype(F32)
    for stream, view in streams:
        for d in range(zs):
            for copy, wanted in hops(stream, view, d):
                pl.when(wanted)(copy.wait_send)
    for d in range(1, zs):
        part_copy(d).wait_send()
    for b in range(2):
        for d in range(zs):
            run(zpeer(0, 1), g_view(b)(d), g_view(b, 1)(d), qxs.at[b, d], qxr.at[b, d]).wait_send()
    for copy in pending:
        copy.wait_send()


def fused(target, gain, w_query, queries, keys, values, attn_out, grad_out):
    zs, ts = lax.axis_size("sp") // X, lax.axis_size("tp")
    rows, width = queries.shape
    src = keys.shape[0]
    heads = width // HEAD_DIM
    cols, hd = heads * rows, HEAD_DIM
    feats = target.shape[1]
    feat = feats // (zs * X)
    part = src // ts
    copies = 6 * zs * X + 8 * ts + 16
    vmem, hbm = pl.BlockSpec(memory_space=pltpu.VMEM), pl.BlockSpec(memory_space=pl.ANY)
    return pl.pallas_call(
        functools.partial(fused_kernel, zs, ts, heads),
        out_shape=(
            jax.ShapeDtypeStruct((rows, feats), BF16),
            jax.ShapeDtypeStruct((feat, width * ts), F32),
            jax.ShapeDtypeStruct((part, keys.shape[1]), F32),
            jax.ShapeDtypeStruct((part, keys.shape[1]), F32),
        ),
        in_specs=[vmem, vmem, hbm, hbm, hbm, hbm, hbm, hbm],
        out_specs=(vmem,) * 4,
        scratch_shapes=[
            pltpu.VMEM((zs, cols, hd), BF16),
            pltpu.VMEM((zs, cols, hd), BF16),
            pltpu.VMEM((cols, hd), BF16),
            pltpu.VMEM((X * src, hd), BF16),
            pltpu.VMEM((X * src, hd), BF16),
            pltpu.VMEM((hd, X * src), BF16),
            pltpu.VMEM((zs, 8, cols), F32),
            pltpu.VMEM((X * src, cols), F32),
            pltpu.VMEM((zs, X * src, cols), BF16),
            pltpu.VMEM((zs, X * src, cols), BF16),
            pltpu.VMEM((zs, hd, cols), BF16),
            pltpu.VMEM((zs, hd, cols), BF16),
            pltpu.VMEM((zs, 8, cols), F32),
            pltpu.VMEM((zs, zs, 8, cols), F32),
            pltpu.VMEM((2, X * src, hd), F32),
            pltpu.VMEM((2, src, hd), BF16),
            pltpu.VMEM((2, src, hd), BF16),
            pltpu.VMEM((2, src, hd), BF16),
            pltpu.VMEM((ts, 2, part, hd), BF16),
            pltpu.VMEM((ts, rows, 128), F32),
            pltpu.VMEM((feats, rows), BF16),
            pltpu.VMEM((ts, feat, zs * X * rows), BF16),
            pltpu.VMEM((rows, width), BF16),
            pltpu.VMEM((2, zs * X * rows, width // 2), BF16),
            pltpu.VMEM((ts, rows, width), BF16),
            pltpu.VMEM((ts, feats, width), BF16),
            pltpu.VMEM((2, ts, feat, width // 2), BF16),
            pltpu.VMEM((2, ts, feat, width // 2), BF16),
            pltpu.SemaphoreType.DMA((copies,)),
            pltpu.SemaphoreType.DMA((copies,)),
            pltpu.SemaphoreType.DMA((2 + 3 * heads + ts,)),
            pltpu.SemaphoreType.DMA((4, zs, 2)),
            pltpu.SemaphoreType.DMA((4, zs)),
            pltpu.SemaphoreType.DMA((zs,)),
            pltpu.SemaphoreType.DMA((zs,)),
            pltpu.SemaphoreType.DMA((2, zs)),
            pltpu.SemaphoreType.DMA((2, zs)),
        ],
        compiler_params=pltpu.CompilerParams(
            collective_id=0, has_side_effects=True, vmem_limit_bytes=60 * 2**20
        ),
    )(target, gain.reshape(1, feats), w_query, queries, keys, values, attn_out, grad_out)


def fits(mesh):
    sp, tp = mesh.shape["sp"], mesh.shape["tp"]
    feat = WIDTH // (sp * tp)
    return tp == KV_HEADS and sp == 4 * X and feat % 128 == 0


def solution(mesh):
    return jax.shard_map(
        fused if fits(mesh) else local,
        mesh=mesh,
        in_specs=(
            P("sp", "tp"),
            P("tp"),
            P("tp", None),
            P("sp", "tp"),
            P("sp", None),
            P("sp", None),
            P("sp", "tp"),
            P("sp", "tp"),
        ),
        out_specs=(
            P("sp", "tp"),
            P(("tp", "sp"), None),
            P(("sp", "tp"), None),
            P(("sp", "tp"), None),
        ),
        check_vma=False,
    )
```

```python
import functools
import math

import jax
import jax.numpy as jnp
from jax import lax
from jax.experimental import pallas as pl
from jax.experimental.pallas import tpu as pltpu
from jax.sharding import PartitionSpec as P

WIDTH = 4096
HEADS = 16
KV_HEADS = 4
HEAD_DIM = 256


norm_eps = 1e-06


def merged(part, axis, combine):
    gathered = jax.tree.map(lambda a: lax.all_gather(a, axis), part)

    def take(source):
        return jax.tree.map(lambda a: lax.dynamic_index_in_dim(a, source, 0, False), gathered)

    return lax.fori_loop(
        1, lax.axis_size(axis), lambda source, state: combine(state, take(source)), take(0)
    )


def join_stats(first_part, second_part):
    row_peak = jnp.maximum(first_part[0], second_part[0])
    summed = first_part[1] * jnp.exp(first_part[0] - row_peak) + second_part[1] * jnp.exp(
        second_part[0] - row_peak
    )
    return (row_peak, summed, first_part[2] + second_part[2])


def local(target, gain, w_query, queries, keys, values, attn_out, grad_out):
    local_heads = queries.shape[1] // HEAD_DIM
    group_size = HEADS // KV_HEADS
    score_scale = HEAD_DIM ** (-0.5)
    own_rows = queries.shape[0]
    src_rows = keys.shape[0]
    kv_index = lax.axis_index("tp") * local_heads // group_size
    key_own = lax.dynamic_slice_in_dim(keys, kv_index * HEAD_DIM, HEAD_DIM, 1)
    value_own = lax.dynamic_slice_in_dim(values, kv_index * HEAD_DIM, HEAD_DIM, 1)
    out_heads = attn_out.reshape(own_rows, local_heads, HEAD_DIM).astype(jnp.float32)
    grad_heads = grad_out.reshape(own_rows, local_heads, HEAD_DIM).astype(jnp.float32)
    delta_own = jnp.sum(out_heads * grad_heads, axis=2)
    empty_sum = jnp.zeros((src_rows, HEAD_DIM), jnp.float32)
    total_rows = own_rows * lax.axis_size("sp")
    position = lax.axis_index("sp") * own_rows
    delta_full = lax.dynamic_update_slice_in_dim(
        jnp.zeros((total_rows, local_heads), jnp.float32), delta_own, position, 0
    )
    query_all, grad_all = (
        lax.all_gather(queries, "sp", axis=0, tiled=True),
        lax.all_gather(grad_out, "sp", axis=0, tiled=True),
    )
    block_rows = math.gcd(total_rows, 512)
    block_count = total_rows // block_rows
    query_blocks = query_all.reshape(block_count, block_rows, local_heads, HEAD_DIM)
    grad_blocks = grad_all.reshape(block_count, block_rows, local_heads, HEAD_DIM)

    def block_stats(query_block):
        scores = (
            jnp.einsum("qhd,sd->hqs", query_block, key_own, preferred_element_type=jnp.float32)
            * score_scale
        )
        row_peak = jnp.max(scores, axis=2)
        row_total = jnp.sum(jnp.exp(scores - row_peak[:, :, None]), axis=2)
        return (row_peak, row_total)

    peaks, totals = lax.map(block_stats, query_blocks)
    peaks, totals, delta_full = merged((peaks, totals, delta_full), "sp", join_stats)
    log_totals = peaks + jnp.log(totals)
    delta_blocks = delta_full.reshape(block_count, block_rows, local_heads)

    def block_grads(running, inputs):
        query_block, grad_block, delta_block, log_block = inputs
        scores = (
            jnp.einsum("qhd,sd->hqs", query_block, key_own, preferred_element_type=jnp.float32)
            * score_scale
        )
        weights = jnp.exp(scores - log_block[:, :, None])
        grad_weights = jnp.einsum(
            "qhd,sd->hqs", grad_block, value_own, preferred_element_type=jnp.float32
        )
        delta_cols = jnp.transpose(delta_block)
        grad_scores = (weights * (grad_weights - delta_cols[:, :, None]) * score_scale).astype(
            jnp.bfloat16
        )
        key_sum = running[0] + jnp.einsum(
            "hqs,qhd->sd", grad_scores, query_block, preferred_element_type=jnp.float32
        )
        value_sum = running[1] + jnp.einsum(
            "hqs,qhd->sd",
            weights.astype(jnp.bfloat16),
            grad_block,
            preferred_element_type=jnp.float32,
        )
        query_part = jnp.einsum(
            "hqs,sd->qhd", grad_scores, key_own, preferred_element_type=jnp.float32
        )
        return ((key_sum, value_sum), query_part)

    (key_sum, value_sum), query_parts = lax.scan(
        block_grads, (empty_sum, empty_sum), (query_blocks, grad_blocks, delta_blocks, log_totals)
    )
    query_parts = query_parts.reshape(total_rows, 1, local_heads * HEAD_DIM)
    received = lax.all_to_all(
        query_parts.astype(jnp.bfloat16), "sp", split_axis=0, concat_axis=1, tiled=True
    ).astype(query_parts.dtype)
    query_grad = jnp.sum(received, axis=1)
    key_cols = key_sum.reshape(src_rows, 1, HEAD_DIM)
    value_cols = value_sum.reshape(src_rows, 1, HEAD_DIM)
    key_parts, value_parts = (
        lax.all_to_all(
            key_cols.astype(jnp.bfloat16), "tp", split_axis=0, concat_axis=1, tiled=True
        ).astype(key_cols.dtype),
        lax.all_to_all(
            value_cols.astype(jnp.bfloat16), "tp", split_axis=0, concat_axis=1, tiled=True
        ).astype(value_cols.dtype),
    )
    part_rows = key_parts.shape[0]
    per_kv = key_parts.shape[1] // KV_HEADS
    grad_keys = (
        key_parts.reshape(part_rows, KV_HEADS, per_kv, HEAD_DIM)
        .sum(axis=2)
        .reshape(part_rows, KV_HEADS * HEAD_DIM)
    )
    grad_values = (
        value_parts.reshape(part_rows, KV_HEADS, per_kv, HEAD_DIM)
        .sum(axis=2)
        .reshape(part_rows, KV_HEADS * HEAD_DIM)
    )
    query_grad = query_grad.astype(jnp.bfloat16)
    query_all_heads = lax.all_gather(query_grad, "tp", axis=1, tiled=True)
    grad_rows = lax.dot_general(
        query_all_heads, w_query, (((1,), (1,)), ((), ())), preferred_element_type=jnp.float32
    ).astype(jnp.bfloat16)
    target_wide = target.astype(jnp.float32)
    squares = lax.psum(jnp.sum(target_wide * target_wide, axis=1), "tp")
    inverse = lax.rsqrt(squares / WIDTH + norm_eps)
    normed = (target_wide * inverse[:, None] * gain).astype(jnp.bfloat16)
    grad_weight = lax.psum_scatter(
        lax.dot_general(
            normed, query_all_heads, (((0,), (0,)), ((), ())), preferred_element_type=jnp.float32
        ).astype(jnp.bfloat16),
        "sp",
        scatter_dimension=0,
        tiled=True,
    ).astype(jnp.float32)
    return (grad_rows, grad_weight, grad_keys, grad_values)


MESH = pl.DeviceIdType.MESH
BF16, F32 = jnp.bfloat16, jnp.float32
NT = (((1,), (1,)), ((), ()))
X = 2
CHUNK = 256


def fused_kernel(
    zs, ts, heads,
    target, gain, w_query, queries, keys, values, attn_out, grad_out,
    grad_rows, grad_weight, grad_keys, grad_values,
    qs, dos, outs, kbuf, vbuf, ktr, delta, sbuf, pbuf, dsbuf, qpart, qpart_in,
    stat, stat_in, ksum, kv_out, kv_in, kv_tp, kv_tp_in, sq, ntr, nall,
    qown, qg, qt, wbuf, res_out, res_in, send, recv, local_sem, zsend, zrecv, psend, precv, qxs, qxr,
):
    rows = queries.shape[0]
    src = keys.shape[0]
    hd = HEAD_DIM
    width = heads * hd
    cols = heads * rows
    part = src // ts
    feat = target.shape[1] // (zs * X)
    scale = hd ** (-0.5)
    sp, tp = lax.axis_index("sp"), lax.axis_index("tp")
    z, x = sp // X, sp % X
    counter = [0]
    pending = []

    def zpeer(d, dx=0):
        return (((z + d) % zs) * X + (x + dx) % X, tp)

    def tpeer(e):
        return (sp, (tp + e) % ts)

    def push(source, dest, device):
        i = counter[0]
        counter[0] += 1
        copy = pltpu.make_async_remote_copy(
            src_ref=source, dst_ref=dest, send_sem=send.at[i], recv_sem=recv.at[i],
            device_id=device, device_id_type=MESH,
        )
        copy.start()
        pending.append(copy)
        return copy

    def run(device, source, dest, ssem, rsem):
        return pltpu.make_async_remote_copy(
            src_ref=source, dst_ref=dest, send_sem=ssem, recv_sem=rsem,
            device_id=device, device_id_type=MESH,
        )

    first = (zs - 1 - z) // (zs - 1)
    last = z // (zs - 1)
    inner = first + last == 0
    near = [1 + 2 * first, 3 - first - last, 2 - first + last]

    def hops(stream, view, d):
        up = run(
            zpeer(1), view(d), view((d + 1) % zs), zsend.at[stream, d, 0],
            zrecv.at[stream, (d + 1) % zs],
        )
        down = run(
            zpeer(zs - 1), view(d), view((d + zs - 1) % zs), zsend.at[stream, d, 1],
            zrecv.at[stream, (d + zs - 1) % zs],
        )
        below, above = z >= d, z < d
        if isinstance(d, int) and d == 0:
            above = z >= 0
        return ((up, below & (z < zs - 1)), (down, above & (z > 0)))

    def forward(stream, view, d):
        for copy, wanted in hops(stream, view, d):
            pl.when(wanted)(copy.start)

    def arrived(stream, view, d):
        run(zpeer(1), view(0), view(d), zsend.at[stream, 0, 0], zrecv.at[stream, d]).wait_recv()

    def relay(stream, view, d):
        arrived(stream, view, d)
        forward(stream, view, d)

    q_view, d_view = (lambda d: qs.at[d]), (lambda d: dos.at[d])
    half = width // 2

    def g_view(b, dx=0):
        return lambda d: qg.at[b, pl.ds(pl.multiple_of((d * X + dx) * rows, rows), rows)]

    streams = ((0, q_view), (1, d_view), (2, g_view(0)), (3, g_view(1)))

    local_count = [0]

    def fetch(source, dest):
        i = local_count[0]
        local_count[0] += 1
        copy = pltpu.make_async_copy(source, dest, local_sem.at[i])
        copy.start()
        return copy

    head_col = pl.ds(pl.multiple_of(tp * hd, hd), hd)
    q_loads, d_loads, o_loads = [], [], []
    kv_loads = [
        fetch(keys.at[:, head_col], kbuf.at[pl.ds(0, src)]),
        fetch(values.at[:, head_col], vbuf.at[pl.ds(0, src)]),
    ]
    for ref, buf, loads in ((queries, qs, q_loads), (grad_out, dos, d_loads), (attn_out, outs, o_loads)):
        for h in range(heads):
            view = buf.at[pl.ds(h * rows, rows)] if buf is outs else buf.at[0, pl.ds(h * rows, rows)]
            loads.append(fetch(ref.at[:, pl.ds(h * hd, hd)], view))
    w_loads = []
    for e in range(ts):
        w_col = pl.ds(pl.multiple_of(((tp + ts - e) % ts) * width, width), width)
        w_loads.append(fetch(w_query.at[:, w_col], wbuf.at[e]))

    barrier = pltpu.get_barrier_semaphore()
    peers = [zpeer(d, dx) for d in range(zs) for dx in range(X) if d + dx]
    peers += [tpeer(e) for e in range(1, ts)]
    for peer in peers:
        pl.semaphore_signal(barrier, inc=1, device_id=peer, device_id_type=MESH)
    pl.semaphore_wait(barrier, len(peers))

    order = [1, zs - 1] + list(range(2, zs - 1)) if zs > 2 else list(range(1, zs))
    for copy in q_loads:
        copy.wait()
    forward(0, q_view, 0)
    for copy in kv_loads:
        copy.wait()
    k_in = push(kbuf.at[pl.ds(0, src)], kbuf.at[pl.ds(src, src)], zpeer(0, 1))
    v_in = push(vbuf.at[pl.ds(0, src)], vbuf.at[pl.ds(src, src)], zpeer(0, 1))
    for copy in d_loads:
        copy.wait()
    forward(1, d_view, 0)

    wide = target[...].astype(F32)
    sq[0] = jnp.broadcast_to(jnp.sum(wide * wide, axis=1, keepdims=True), (rows, 128))
    sq_in = [push(sq.at[0], sq.at[e], tpeer(e)) for e in range(1, ts)]

    for copy in o_loads:
        copy.wait()
    for h in range(heads):
        span = pl.ds(h * rows, rows)
        dot = jnp.sum(dos[0, span].astype(F32) * outs[span].astype(F32), axis=1, keepdims=True)
        delta[0, :, span] = jnp.broadcast_to(dot, (rows, 128)).T[:8]
    delta_in = {d: push(delta.at[0], delta.at[d], zpeer(d)) for d in order}

    for copy in sq_in:
        copy.wait_recv()
    total = sq[0]
    for e in range(1, ts):
        total = total + sq[e]
    inverse = lax.rsqrt(total[:, :1] / (target.shape[1] * ts) + norm_eps)
    normed = target[...].astype(F32) * inverse * gain[...]
    ntr[...] = normed.T.astype(BF16)

    def feature_rows(d, dx):
        owner = ((z + d) % zs) * X + (x + dx) % X
        return pl.ds(pl.multiple_of(owner * feat, feat), feat)

    n_in = []
    for d in range(zs):
        for dx in range(X):
            lanes = pl.ds((d * X + dx) * rows, rows)
            if d + dx:
                n_in.append(
                    push(ntr.at[feature_rows(d, dx)], nall.at[0, :, lanes], zpeer(d, dx))
                )
            else:
                nall[0, :, lanes] = ntr[feature_rows(0, 0)]

    chunks = X * src // CHUNK

    def scores_of(d):
        def step(c, peak):
            span = pl.ds(pl.multiple_of(c * CHUNK, CHUNK), CHUNK)
            s = lax.dot_general(kbuf[span], qs[d], NT, preferred_element_type=F32)
            sbuf[span] = s
            return jnp.maximum(peak, jnp.max(s, axis=0, keepdims=True))

        return lax.fori_loop(0, chunks, step, jnp.full((1, cols), -jnp.inf, F32))

    def grads_of(d, peak):
        own_delta = delta[d, :1]

        def step(c, total):
            span = pl.ds(pl.multiple_of(c * CHUNK, CHUNK), CHUNK)
            p = jnp.exp((sbuf[span] - peak) * scale)
            dp = lax.dot_general(vbuf[span], dos[d], NT, preferred_element_type=F32)
            pbuf[d, span] = p.astype(BF16)
            dsbuf[d, span] = (p * (dp - own_delta) * scale).astype(BF16)
            return total + jnp.sum(p, axis=0, keepdims=True)

        total = lax.fori_loop(0, chunks, step, jnp.zeros((1, cols), F32))
        stat[d, 0:1] = peak * scale
        stat[d, 1:2] = total
        stat[d, 2:8] = jnp.zeros((6, cols), F32)
        return jnp.dot(ktr[...], dsbuf[d], preferred_element_type=F32)

    def process(d):
        peak = scores_of(d)
        qpart[d] = grads_of(d, peak).astype(BF16)

    def part_copy(d):
        return run(zpeer(zs - d), qpart.at[d], qpart_in.at[d], psend.at[d], precv.at[d])

    relay(0, q_view, near[0])
    ktr[:, :src] = kbuf[:src].T
    k_in.wait_recv()
    ktr[:, src:] = kbuf[src:].T
    relay(1, d_view, near[0])
    v_in.wait_recv()

    @pl.when(inner)
    def _():
        relay(0, q_view, near[1])
        relay(1, d_view, near[1])

    for copy in delta_in.values():
        copy.wait_recv()
    process(0)

    @pl.when(inner)
    def _():
        relay(0, q_view, near[2])

    process(near[0])
    part_copy(near[0]).start()

    @pl.when(inner)
    def _():
        relay(1, d_view, near[2])

    @pl.when(first + last > 0)
    def _():
        arrived(0, q_view, near[1])
        arrived(1, d_view, near[1])

    process(near[1])
    part_copy(near[1]).start()

    @pl.when(first + last > 0)
    def _():
        arrived(0, q_view, near[2])
        arrived(1, d_view, near[2])

    process(near[2])
    part_copy(near[2]).start()
    for copy in n_in:
        copy.wait_recv()
    nt_in = [push(nall.at[0], nall.at[e], tpeer(e)) for e in range(1, ts)]

    stat_copies = [push(stat, stat_in.at[d], zpeer(d)) for d in order]
    for copy in stat_copies:
        copy.wait_recv()

    def stats_of(d, e):
        ref = stat.at[d] if e == 0 else stat_in.at[e, (d + zs - e) % zs]
        return ref[0:1], ref[1:2]

    def ratios(d):
        parts = [stats_of(d, e) for e in range(zs)]
        top = parts[0][0]
        for m, _ in parts[1:]:
            top = jnp.maximum(top, m)
        factors = [jnp.exp(m - top) for m, _ in parts]
        summed = sum(f * l for f, (_, l) in zip(factors, parts))
        return [f / summed for f in factors]

    own_ratios = ratios(0)
    for d in range(zs):
        r = own_ratios[0] if d == 0 else ratios(d)[0]
        r = jnp.broadcast_to(r, (128, cols)).T
        r = jnp.concatenate([r] * (hd // 128), axis=1)
        sbuf_q = (qs[d].astype(F32) * r).astype(BF16)
        sbuf_d = (dos[d].astype(F32) * r).astype(BF16)
        for i, (left, right) in enumerate(((dsbuf, sbuf_q), (pbuf, sbuf_d))):
            piece = jnp.dot(left[d], right, preferred_element_type=F32)
            ksum[i] = piece if d == 0 else ksum[i] + piece
    kv_out[...] = ksum[:, src:].astype(BF16)
    kvx_in = push(kv_out, kv_in, zpeer(0, 1))

    grad_t = qpart[0].astype(F32) * own_ratios[0]
    for d in order:
        part_copy(d).wait_recv()
        grad_t = grad_t + qpart_in[d].astype(F32) * own_ratios[(zs - d) % zs]
    grad_own = grad_t.T
    for h in range(heads):
        piece = grad_own[h * rows : (h + 1) * rows].astype(BF16)
        qown[:, pl.ds(h * hd, hd)] = piece
        b, at = h * hd // half, h * hd % half
        qg[b, pl.ds(0, rows), pl.ds(at, hd)] = piece
    def cross(b, d):
        run(zpeer(0, 1), g_view(b)(d), g_view(b, 1)(d), qxs.at[b, d], qxr.at[b, d]).start()

    forward(2, g_view(0), 0)
    cross(0, 0)
    qt_in = {e: push(qown, qt.at[e], tpeer(e)) for e in range(1, ts)}
    relay(2, g_view(0), near[0])
    forward(3, g_view(1), 0)
    cross(0, near[0])
    cross(1, 0)

    kvx_in.wait_recv()
    for i in range(2):
        ksum[i, :src] = ksum[i, :src] + kv_in[i].astype(F32)
    kv_tp[...] = ksum[:, :src].astype(BF16)

    def part_rows(e):
        return pl.ds(pl.multiple_of(((tp + e) % ts) * part, part), part)

    kvt_in = [push(kv_tp.at[:, part_rows(e)], kv_tp_in.at[e], tpeer(e)) for e in range(1, ts)]
    for i, out in enumerate((grad_keys, grad_values)):
        out[:, head_col] = ksum[i, part_rows(0)]

    w_loads[0].wait()
    rows_sum = lax.dot_general(qown[...], wbuf[0], NT, preferred_element_type=F32)
    relay(2, g_view(0), near[1])
    cross(0, near[1])
    relay(3, g_view(1), near[0])
    cross(1, near[0])
    relay(2, g_view(0), near[2])
    cross(0, near[2])
    relay(3, g_view(1), near[1])
    cross(1, near[1])
    for e in range(1, ts):
        kvt_in[e - 1].wait_recv()
        at = pl.ds(pl.multiple_of(((tp + ts - e) % ts) * hd, hd), hd)
        for i, out in enumerate((grad_keys, grad_values)):
            out[:, at] = kv_tp_in[e, i].astype(F32)
    for copy in nt_in:
        copy.wait_recv()
    def crossed(b):
        for d in range(zs):
            run(zpeer(0, 1), g_view(b)(d), g_view(b, 1)(d), qxs.at[b, d], qxr.at[b, d]).wait_recv()

    res_copies = {}

    def project(b):
        for e in [*range(1, ts), 0]:
            piece = jnp.dot(nall[e], qg[b], preferred_element_type=F32)
            if e:
                res_out[b, e] = piece.astype(BF16)
                res_copies[b, e] = push(res_out.at[b, e], res_in.at[b, e], tpeer(ts - e))
            else:
                grad_weight[:, pl.ds(pl.multiple_of(tp * width + b * half, half), half)] = piece

    crossed(0)
    project(0)
    relay(3, g_view(1), near[2])
    cross(1, near[2])
    for e in range(1, ts):
        qt_in[e].wait_recv()
        w_loads[e].wait()
        rows_sum = rows_sum + lax.dot_general(qt[e], wbuf[e], NT, preferred_element_type=F32)
    grad_rows[...] = rows_sum.astype(BF16)
    crossed(1)
    project(1)
    for b in range(2):
        for e in range(1, ts):
            res_copies[b, e].wait_recv()
            at = ((tp + e) % ts) * width + b * half
            grad_weight[:, pl.ds(pl.multiple_of(at, half), half)] = res_in[b, e].astype(F32)
    for stream, view in streams:
        for d in range(zs):
            for copy, wanted in hops(stream, view, d):
                pl.when(wanted)(copy.wait_send)
    for d in range(1, zs):
        part_copy(d).wait_send()
    for b in range(2):
        for d in range(zs):
            run(zpeer(0, 1), g_view(b)(d), g_view(b, 1)(d), qxs.at[b, d], qxr.at[b, d]).wait_send()
    for copy in pending:
        copy.wait_send()


def hand_over(*refs):
    for source, dest in zip(refs[:4], refs[4:]):
        dest[...] = source[...]


def fused(target, gain, w_query, queries, keys, values, attn_out, grad_out):
    zs, ts = lax.axis_size("sp") // X, lax.axis_size("tp")
    rows, width = queries.shape
    src = keys.shape[0]
    heads = width // HEAD_DIM
    cols, hd = heads * rows, HEAD_DIM
    feats = target.shape[1]
    feat = feats // (zs * X)
    part = src // ts
    copies = 6 * zs * X + 8 * ts + 16
    vmem, hbm = pl.BlockSpec(memory_space=pltpu.VMEM), pl.BlockSpec(memory_space=pl.ANY)
    results = pl.pallas_call(
        functools.partial(fused_kernel, zs, ts, heads),
        out_shape=(
            jax.ShapeDtypeStruct((rows, feats), BF16),
            jax.ShapeDtypeStruct((feat, width * ts), F32),
            jax.ShapeDtypeStruct((part, keys.shape[1]), F32),
            jax.ShapeDtypeStruct((part, keys.shape[1]), F32),
        ),
        in_specs=[vmem, vmem, hbm, hbm, hbm, hbm, hbm, hbm],
        out_specs=(vmem,) * 4,
        scratch_shapes=[
            pltpu.VMEM((zs, cols, hd), BF16),
            pltpu.VMEM((zs, cols, hd), BF16),
            pltpu.VMEM((cols, hd), BF16),
            pltpu.VMEM((X * src, hd), BF16),
            pltpu.VMEM((X * src, hd), BF16),
            pltpu.VMEM((hd, X * src), BF16),
            pltpu.VMEM((zs, 8, cols), F32),
            pltpu.VMEM((X * src, cols), F32),
            pltpu.VMEM((zs, X * src, cols), BF16),
            pltpu.VMEM((zs, X * src, cols), BF16),
            pltpu.VMEM((zs, hd, cols), BF16),
            pltpu.VMEM((zs, hd, cols), BF16),
            pltpu.VMEM((zs, 8, cols), F32),
            pltpu.VMEM((zs, zs, 8, cols), F32),
            pltpu.VMEM((2, X * src, hd), F32),
            pltpu.VMEM((2, src, hd), BF16),
            pltpu.VMEM((2, src, hd), BF16),
            pltpu.VMEM((2, src, hd), BF16),
            pltpu.VMEM((ts, 2, part, hd), BF16),
            pltpu.VMEM((ts, rows, 128), F32),
            pltpu.VMEM((feats, rows), BF16),
            pltpu.VMEM((ts, feat, zs * X * rows), BF16),
            pltpu.VMEM((rows, width), BF16),
            pltpu.VMEM((2, zs * X * rows, width // 2), BF16),
            pltpu.VMEM((ts, rows, width), BF16),
            pltpu.VMEM((ts, feats, width), BF16),
            pltpu.VMEM((2, ts, feat, width // 2), BF16),
            pltpu.VMEM((2, ts, feat, width // 2), BF16),
            pltpu.SemaphoreType.DMA((copies,)),
            pltpu.SemaphoreType.DMA((copies,)),
            pltpu.SemaphoreType.DMA((2 + 3 * heads + ts,)),
            pltpu.SemaphoreType.DMA((4, zs, 2)),
            pltpu.SemaphoreType.DMA((4, zs)),
            pltpu.SemaphoreType.DMA((zs,)),
            pltpu.SemaphoreType.DMA((zs,)),
            pltpu.SemaphoreType.DMA((2, zs)),
            pltpu.SemaphoreType.DMA((2, zs)),
        ],
        compiler_params=pltpu.CompilerParams(
            collective_id=0, has_side_effects=True, vmem_limit_bytes=60 * 2**20
        ),
    )(target, gain.reshape(1, feats), w_query, queries, keys, values, attn_out, grad_out)
    return pl.pallas_call(
        hand_over,
        out_shape=tuple(jax.ShapeDtypeStruct(r.shape, r.dtype) for r in results),
        in_specs=[vmem] * 4,
        out_specs=(vmem,) * 4,
        compiler_params=pltpu.CompilerParams(vmem_limit_bytes=16 * 2**20),
    )(*results)


def fits(mesh):
    sp, tp = mesh.shape["sp"], mesh.shape["tp"]
    feat = WIDTH // (sp * tp)
    return tp == KV_HEADS and sp == 4 * X and feat % 128 == 0


def solution(mesh):
    return jax.shard_map(
        fused if fits(mesh) else local,
        mesh=mesh,
        in_specs=(
            P("sp", "tp"),
            P("tp"),
            P("tp", None),
            P("sp", "tp"),
            P("sp", None),
            P("sp", None),
            P("sp", "tp"),
            P("sp", "tp"),
        ),
        out_specs=(
            P("sp", "tp"),
            P(("tp", "sp"), None),
            P(("sp", "tp"), None),
            P(("sp", "tp"), None),
        ),
        check_vma=False,
    )
```
